32 devices in a mesh: grp: 2 (over y), ep: 4 (over z), tp: 4 (over x, core).
Axes of the slice: x: 2, y: 2, z: 4, core: 2. Of those that a mesh axis runs over, the one named last changes fastest.
Arguments:
- query_plain: bfloat16 [2048, 512], P(('grp', 'ep'), 'tp'), parts along dimension 0, may hold values from -400 to 400
- query_rotary: bfloat16 [2048, 256], P(('grp', 'ep'), 'tp'), parts along dimension 0, may hold values from -6 to 6
- latent_input: bfloat16 [2048, 256], P(('grp', 'ep')), parts along dimension 0, may hold values from -6 to 6
- rotary_key: bfloat16 [2048, 32], P(('grp', 'ep')), parts along dimension 0, may hold values from -6 to 6
- key_weight: bfloat16 [256, 512], P(None, 'tp'), may hold values from -0.375 to 0.375
- value_weight: bfloat16 [256, 512], P(None, 'tp'), may hold values from -0.375 to 0.375
- latent_gain: bfloat16 [256], replicated, may hold values from 0.099609375 to 1.8984375
- head_gain: bfloat16 [512], P('tp'), may hold values from 0.099609375 to 1.8984375
- out_weight: bfloat16 [512, 2048], P('tp'), may hold values from -0.25 to 0.25
- expert_input: bfloat16 [4096, 2048], P(('grp', 'ep', 'tp')), parts along dimension 0, may hold values from -6 to 6
- expert_gain: bfloat16 [2048], replicated, may hold values from 0.099609375 to 1.8984375
- routes: int32 [4096, 2], P(('grp', 'ep', 'tp')), parts along dimension 0, may hold values from 0 to 3, all different within a row; in each aligned block of 128 rows (0 to 127, 128 to 255, ...) at most 72 rows name the same one
- route_weight: float32 [4096, 2], P(('grp', 'ep', 'tp')), parts along dimension 0, may hold values from 0.1 to 1
- gate_weight: bfloat16 [4, 2048, 3584], P('ep', None, 'tp'), may hold values from -0.125 to 0.125
- up_weight: bfloat16 [4, 2048, 3584], P('ep', None, 'tp'), may hold values from -0.125 to 0.125
- down_weight: bfloat16 [4, 3584, 2048], P('ep', 'tp'), may hold values from -0.09375 to 0.09375
Outputs:
- attended: bfloat16 [2048, 2048], P(('grp', 'ep', 'tp')), parts along dimension 0
- expert_out: bfloat16 [4096, 2048], P(('grp', 'ep', 'tp')), parts along dimension 0
The draws below stay inside these ranges and needn't reach their ends.
There are 2 independent parts, one for each index of `grp`. The reference program is written for one: setup_inputs(seed, part) draws one part's arguments, and reference() takes and returns one part's arrays. A program takes and returns all parts, laid end to end along the dimension named above; an argument that names none is the same for every part. Nothing has to cross between parts.
Inputs may be any that keep to these rules, and one draw needn't show every extreme that they name: `routes`: each of the 128 rows of one device names 2 different experts; no expert is named by more than 72 rows of one device, a bound that some block reaches of some device.
All inputs are finite; a program needn't handle non-finite values.
Results may differ from the reference program's by a relative error of at most 0.012.
Values may be sent and summed in bfloat16 or wider, within the bound.
A program may use at most 128 MiB of HBM per device.

```python
import math
import jax
import jax.numpy as jnp
import numpy as np
from jax import lax

D = 2048
HEADS = 8
PLAIN_DIM = 64
ROTARY_DIM = 32
VALUE_DIM = 64
LATENT = 256
FF = 3584
TOP = 2
TOK_A = 256
TOK_B = 128
EXPERTS = 4
CAP = 72
TOKENS_A = 1024
TOKENS_B = 2048
N_EP = 4
N_TP = 4


def draw_query_plain(key, part):
    first = jax.random.fold_in(key, 0)
    shape = (TOKENS_A, HEADS * PLAIN_DIM)
    return jnp.clip(jax.random.normal(first, shape, jnp.float32), -5.0, 5.0).astype(jnp.bfloat16)


def block_levels(key, dims, shards, least, largest):
    def one(axis_at, parts):
        steps = jax.random.uniform(jax.random.fold_in(jax.random.fold_in(key, 6), axis_at), (parts,), jnp.float32, least / len(shards), largest / len(shards))
        return jnp.repeat(jnp.exp(steps), dims[axis_at] // parts).reshape((-1,) + (1,) * (len(dims) - axis_at - 1))

    loudness = one(*shards[0])
    for cut in shards[1:]:
        loudness = loudness * one(*cut)
    return loudness


def deal_out(stream_key, own, number, rows, number_of, top, limit, slope):
    ranking = jax.random.permutation(stream_key, number_of)
    crowded, ordinary = portions_of(number_of, rows * top, limit, slope, True), portions_of(number_of, rows * top, limit, slope, False)
    places = jnp.arange(number_of)

    def named(sizes, rotation):
        used = int((sizes > 0).sum())
        fixed = max(1, used // 4)
        shifted = fixed + (places - fixed + rotation * (used - fixed)) % max(1, number_of - fixed)
        return jnp.zeros((number_of,), jnp.int32).at[ranking[jnp.where(places < fixed, places, shifted)]].set(jnp.asarray(sizes, jnp.int32))

    sizes = jnp.where(number % 4 == 0, named(crowded, number // 4), named(ordinary, number - number // 4 - 1))
    mixed = jax.random.permutation(jax.random.fold_in(own, 3), number_of)
    donor, sink = mixed[0:number_of // 2 * 2:2], mixed[1:number_of // 2 * 2:2]
    slack = jnp.minimum(sizes[donor] - 1, limit - sizes[sink]) // 2
    slack = jnp.where((donor == ranking[0]) | (sink == ranking[0]) | (sizes[sink] == 0), 0, jnp.maximum(slack, 0))
    shifted = jax.random.randint(jax.random.fold_in(own, 4), (number_of // 2,), 0, 1 << 20) % (slack + 1)
    sizes = sizes.at[donor].add(-shifted).at[sink].add(shifted)
    items = jnp.searchsorted(jnp.cumsum(sizes), jnp.arange(rows * top), side="right").astype(jnp.int32)
    grid = items.reshape(top, rows).T
    grid = grid[jax.random.permutation(jax.random.fold_in(own, 1), rows)]
    rotation = jax.random.randint(jax.random.fold_in(own, 2), (rows, 1), 0, top)
    return jnp.take_along_axis(grid, (jnp.arange(top)[None, :] + rotation) % top, axis=1)


def portions_of(number_of, total, limit, lean, full):
    loads = [(1 << 20) // math.isqrt(standing ** lean) + 1 for standing in range(1, number_of + 1)]
    largest = limit if full else min(limit, max(-(-total // number_of), total * loads[0] // sum(loads)))
    least = 1 if total - largest >= number_of - 1 else 0
    holding, rest = [largest] + [least] * (number_of - 1), total - largest - least * (number_of - 1)
    while rest > 0:
        free = [i for i in range(1, number_of) if holding[i] < largest] or [i for i in range(1, number_of) if holding[i] < limit]
        whole, budget = sum([loads[i] for i in free]), rest
        for i in free:
            extra = min(limit - holding[i], max(1, budget * loads[i] // whole), rest)
            holding[i] = holding[i] + extra
            rest = rest - extra
    return np.array(holding)


def normal_values(key, extent, scale, reach, pieces=(), kind=jnp.bfloat16):
    array = jax.random.normal(key, extent, jnp.float32) * scale
    if len(pieces) > 0:
        array = block_levels(key, extent, pieces, -0.22, 0.18) * array
    return jnp.clip(array, min=-reach, max=reach).astype(kind)


def setup_inputs(seed: int = 0, part: int = 0) -> dict:
    arg_keys = jax.random.split(jax.random.key(seed), 17)
    part_splits = jax.random.split(jax.random.fold_in(arg_keys[16], part), 17)
    query_plain = draw_query_plain(jax.random.fold_in(jax.random.fold_in(arg_keys[16], part), 71), part)
    query_rotary = normal_values(part_splits[1], (TOKENS_A, HEADS * ROTARY_DIM), 1.0, 6.0, ((0, 4), (1, 4)))
    latent_input = normal_values(part_splits[2], (TOKENS_A, LATENT), 1.0, 6.0, ((0, 4),))
    rotary_key = normal_values(part_splits[3], (TOKENS_A, ROTARY_DIM), 1.0, 6.0, ((0, 4),))
    key_weight = normal_values(arg_keys[4], (LATENT, HEADS * PLAIN_DIM), LATENT ** -0.5, 0.375, ((1, 4),))
    value_weight = normal_values(arg_keys[5], (LATENT, HEADS * VALUE_DIM), LATENT ** -0.5, 0.375, ((1, 4),))
    latent_gain = jnp.clip(1.0 + 0.18 * jax.random.normal(arg_keys[6], (LATENT,), jnp.float32), 0.099609375, 1.8984375).astype(jnp.bfloat16)
    head_gain = jnp.clip(1.0 + 0.18 * jax.random.normal(arg_keys[7], (HEADS * VALUE_DIM,), jnp.float32), 0.099609375, 1.8984375).astype(jnp.bfloat16)
    out_weight = normal_values(arg_keys[8], (HEADS * VALUE_DIM, D), (HEADS * VALUE_DIM) ** -0.5, 0.25, ((0, 4),))
    expert_input = normal_values(part_splits[9], (TOKENS_B, D), 1.0, 6.0, ((0, 16),))
    expert_gain = jnp.clip(1.0 + 0.18 * jax.random.normal(arg_keys[10], (D,), jnp.float32), 0.099609375, 1.8984375).astype(jnp.bfloat16)
    routes_keys = jax.random.split(jax.random.fold_in(part_splits[11], 1), TOKENS_B // TOK_B)
    routes_turns = jax.random.permutation(jax.random.fold_in(part_splits[11], 3), TOKENS_B // TOK_B)
    routes = jax.vmap(lambda own, number: deal_out(jax.random.fold_in(part_splits[11], 2), own, number, TOK_B, EXPERTS, TOP, CAP, 1))(routes_keys, routes_turns).reshape((TOKENS_B, TOP))
    route_weight = jnp.clip(0.1 + 0.9 * jax.random.uniform(part_splits[12], (TOKENS_B, TOP), jnp.float32) ** block_levels(part_splits[12], (TOKENS_B, TOP), ((0, 16),), -0.2, 0.2), 0.1, 1.0)
    gate_weight = normal_values(arg_keys[13], (EXPERTS, D, FF), D ** -0.5, 0.125, ((0, 4), (2, 4)))
    up_weight = normal_values(arg_keys[14], (EXPERTS, D, FF), D ** -0.5, 0.125, ((0, 4), (2, 4)))
    down_weight = normal_values(arg_keys[15], (EXPERTS, FF, D), FF ** -0.5, 0.09375, ((0, 4), (1, 4)))
    return dict(query_plain=query_plain, query_rotary=query_rotary, latent_input=latent_input, rotary_key=rotary_key, key_weight=key_weight, value_weight=value_weight, latent_gain=latent_gain, head_gain=head_gain, out_weight=out_weight, expert_input=expert_input, expert_gain=expert_gain, routes=routes, route_weight=route_weight, gate_weight=gate_weight, up_weight=up_weight, down_weight=down_weight)


EPSILON = 1e-06
THETA = 10000.0

def normalize(entries, gain):
    wide = entries.astype(jnp.float32)
    factor = lax.rsqrt(lax.optimization_barrier(jnp.mean(wide * wide, axis=-1, keepdims=True)) + EPSILON)
    return wide * factor * gain.astype(jnp.float32)

def rotate(entries, positions):
    half = entries.shape[-1] // 2
    freqs = THETA ** (-jnp.arange(half, dtype=jnp.float32) / half)
    angle = positions.astype(jnp.float32)[:, None, None] * freqs[None, None, :]
    cosine = jnp.cos(angle)
    sine = jnp.sin(angle)
    first = entries[..., :half].astype(jnp.float32)
    second = entries[..., half:].astype(jnp.float32)
    turned = jnp.concatenate([first * cosine - second * sine, first * sine + second * cosine], axis=-1)
    return turned.astype(jnp.bfloat16)

def rounded(entries):
    return lax.optimization_barrier(entries.astype(jnp.bfloat16)).astype(jnp.float32)

def reference(query_plain, query_rotary, latent_input, rotary_key, key_weight, value_weight, latent_gain, head_gain, out_weight, expert_input, expert_gain, routes, route_weight, gate_weight, up_weight, down_weight):
    positions = jnp.arange(TOKENS_A, dtype=jnp.int32)
    latent = normalize(latent_input, latent_gain).astype(jnp.bfloat16)
    key_rotated = rotate(rotary_key.reshape(TOKENS_A, 1, ROTARY_DIM), positions).reshape(TOKENS_A, ROTARY_DIM)
    query_rotated = rotate(query_rotary.reshape(TOKENS_A, HEADS, ROTARY_DIM), positions)
    keys = jnp.dot(latent, key_weight, preferred_element_type=jnp.float32).astype(jnp.bfloat16)
    values = jnp.dot(latent, value_weight, preferred_element_type=jnp.float32).astype(jnp.bfloat16)
    keys_wide = keys.astype(jnp.float32).reshape(TOKENS_A, HEADS, PLAIN_DIM)
    values_wide = values.astype(jnp.float32).reshape(TOKENS_A, HEADS, VALUE_DIM)
    rotated_wide = key_rotated.astype(jnp.float32)
    queries = query_plain.reshape(TOKENS_A, HEADS, PLAIN_DIM)
    factor = (PLAIN_DIM + ROTARY_DIM) ** (-0.5)

    def attend(block):
        start = (block * TOK_A).astype(jnp.int32)
        query_block = lax.dynamic_slice_in_dim(queries, start, TOK_A, 0).astype(jnp.float32)
        turned_block = lax.dynamic_slice_in_dim(query_rotated, start, TOK_A, 0).astype(jnp.float32)
        scores = jnp.einsum('qhd,khd->hqk', query_block, keys_wide) + jnp.einsum('qhr,kr->hqk', turned_block, rotated_wide)
        scores = scores * factor
        query_positions = start + jnp.arange(TOK_A, dtype=jnp.int32)
        allowed = (positions[None, :] <= query_positions[:, None])[None]
        masked = jnp.where(allowed, scores, -jnp.inf)
        highest = lax.optimization_barrier(jnp.max(masked, axis=-1, keepdims=True))
        weights = jnp.where(allowed, jnp.exp(masked - highest), 0.0).astype(jnp.bfloat16)
        return jnp.einsum('hqk,khd->qhd', weights.astype(jnp.float32), values_wide)
    context = lax.map(attend, jnp.arange(N_EP, dtype=jnp.int32)).reshape(TOKENS_A, HEADS, VALUE_DIM)
    head_output = normalize(context, head_gain.reshape(HEADS, VALUE_DIM)).astype(jnp.bfloat16).reshape(TOKENS_A, HEADS * VALUE_DIM)
    group = HEADS * VALUE_DIM // N_TP
    attended = jnp.zeros((TOKENS_A, D), jnp.float32)
    for index in range(N_TP):
        attended = attended + rounded(jnp.dot(head_output[:, index * group:(index + 1) * group], out_weight[index * group:(index + 1) * group], preferred_element_type=jnp.float32))
    attended = attended.astype(jnp.bfloat16)
    normed = normalize(expert_input, expert_gain).astype(jnp.bfloat16)
    blocks = N_EP * N_TP
    chosen = routes.reshape(blocks, TOK_B * TOP)
    onehot = (chosen[:, :, None] == jnp.arange(EXPERTS, dtype=jnp.int32)[None, None, :]).astype(jnp.int32)
    ranks = lax.optimization_barrier(jnp.sum(jnp.cumsum(onehot, axis=1) * onehot, axis=2)) - 1
    sources = jnp.arange(blocks, dtype=jnp.int32)[:, None]
    slot_index = (chosen * (blocks * CAP) + sources * CAP + ranks).reshape(-1).astype(jnp.int32)
    buffer = jnp.zeros((EXPERTS * blocks * CAP, D), jnp.bfloat16).at[slot_index].set(jnp.repeat(normed, TOP, axis=0))
    buffer = buffer.reshape(EXPERTS, blocks * CAP, D)
    width = FF // N_TP

    def run_expert(inputs):
        expert_rows, gate_local, up_local, down_local = inputs
        gate = jnp.dot(expert_rows, gate_local, preferred_element_type=jnp.float32)
        upward = jnp.dot(expert_rows, up_local, preferred_element_type=jnp.float32)
        expert_hidden = (jax.nn.silu(gate) * upward).astype(jnp.bfloat16)
        result = jnp.zeros((expert_rows.shape[0], D), jnp.float32)
        for index in range(N_TP):
            result = result + rounded(jnp.dot(expert_hidden[:, index * width:(index + 1) * width], down_local[index * width:(index + 1) * width], preferred_element_type=jnp.float32))
        return result.astype(jnp.bfloat16)
    results = lax.map(run_expert, (buffer, gate_weight, up_weight, down_weight)).reshape(EXPERTS * blocks * CAP, D)
    picked = results[slot_index].astype(jnp.float32).reshape(TOKENS_B, TOP, D)
    expert_out = lax.optimization_barrier(jnp.sum(picked * route_weight.astype(jnp.float32)[:, :, None], axis=1)).astype(jnp.bfloat16)
    return (attended, expert_out)
```

```python
import functools
import jax
import jax.numpy as jnp
from jax import lax
from jax.experimental import pallas as pl
from jax.experimental.pallas import tpu as pltpu
from jax.sharding import PartitionSpec as P

PLAIN_DIM = 64
ROTARY_DIM = 32
VALUE_DIM = 64
EPSILON = 1e-06
THETA = 10000.0
LOWEST = -1e30
LANES = 128
MESH = pl.DeviceIdType.MESH
F32 = jnp.float32
BF16 = jnp.bfloat16


def normalize(entries, gain):
    wide = entries.astype(F32)
    factor = lax.rsqrt(jnp.mean(wide * wide, axis=-1, keepdims=True) + EPSILON)
    return wide * factor * gain.astype(F32)


def rotate(entries, positions):
    half = entries.shape[-1] // 2
    freqs = THETA ** (-jnp.arange(half, dtype=F32) / half)
    angle = positions.astype(F32)[:, None, None] * freqs[None, None, :]
    cosine = jnp.cos(angle)
    sine = jnp.sin(angle)
    first = entries[..., :half].astype(F32)
    second = entries[..., half:].astype(F32)
    turned = jnp.concatenate(
        [first * cosine - second * sine, first * sine + second * cosine], axis=-1
    )
    return turned.astype(BF16)


def kernel(
    dims,
    x_ref, gain_ref, routes_ref, weight_ref, lat_ref, q_ref, qr_ref, kw_ref, vw_ref,
    hgain_ref, ow_ref, gate_hbm, up_hbm, down_hbm,
    att_ref, out_ref,
    wgu, wd, outgo, rows, part, hidden, near, pair, across, done, back,
    lats, total, highest, head_part, head_near, head_pair, head_across,
    w_sem, z_send, z_recv, fx_send, fx_recv, fc_send, fc_recv, fd_send, fd_recv,
    n_send, n_recv, a_send, a_recv, b_send, b_recv,
    lz_send, lz_recv, lx_send, lx_recv, lc_send, lc_recv, ld_send, ld_recv,
    h_send, h_recv, i_send, i_recv,
):
    n_ep, n_tp, cap = dims
    tokens = x_ref.shape[0]
    features = x_ref.shape[1]
    tiles = wgu.shape[0]
    pitch = rows.shape[2]
    outer = n_tp // 2
    e = lax.axis_index("ep")
    t = lax.axis_index("tp")
    core = lax.rem(t, 2)
    side = t // 2
    mate = t + 1 - 2 * core
    over = lax.rem(t + 2, n_tp)
    mine = core * outer + side
    mine_over = core * outer + (1 - side)
    sent = pl.ds(0, cap)

    def peer(k):
        return lax.bitwise_xor(e, k)

    def remote(src, dst, send, recv, where):
        return pltpu.make_async_remote_copy(
            src_ref=src, dst_ref=dst, send_sem=send, recv_sem=recv,
            device_id=where, device_id_type=MESH,
        )

    def tile_copies(n):
        columns = pl.ds(n * LANES, LANES)
        return (
            pltpu.make_async_copy(
                gate_hbm.at[0, :, columns], wgu.at[n, :, pl.ds(0, LANES)], w_sem.at[2 * n]
            ),
            pltpu.make_async_copy(
                up_hbm.at[0, :, columns], wgu.at[n, :, pl.ds(LANES, LANES)], w_sem.at[2 * n + 1]
            ),
        )

    down_copy = pltpu.make_async_copy(down_hbm.at[0], wd, w_sem.at[2 * tiles])
    for n in range(tiles):
        for copy in tile_copies(n):
            copy.start()
    down_copy.start()

    barrier = pltpu.get_barrier_semaphore()

    @pl.loop(1, n_ep)
    def _(k):
        pl.semaphore_signal(barrier, inc=1, device_id={"ep": peer(k)}, device_id_type=MESH)

    for where in (mate, over):
        pl.semaphore_signal(barrier, inc=1, device_id={"tp": where}, device_id_type=MESH)
    pl.semaphore_wait(barrier, n_ep + 1)

    def lat_z(k, slot):
        return remote(lat_ref, lats.at[slot, t], lz_send.at[k], lz_recv.at[k], {"ep": peer(k)})

    def lat_x(s, src):
        return remote(src, lats.at[s, t], lx_send.at[s], lx_recv.at[s], {"tp": over})

    def lat_c(s, src):
        return remote(src, lats.at[s, t], lc_send.at[s], lc_recv.at[s], {"tp": mate})

    def lat_d(s):
        return remote(
            lats.at[s, over], lats.at[s, over], ld_send.at[s], ld_recv.at[s], {"tp": mate}
        )

    @pl.loop(1, n_ep)
    def _(k):
        lat_z(k, e).start()

    lat_x(e, lat_ref).start()
    lat_c(e, lat_ref).start()
    lats[e, t] = lat_ref[...]

    wide = x_ref[...].astype(F32)
    factor = lax.rsqrt(jnp.mean(wide * wide, axis=-1, keepdims=True) + EPSILON)
    normed = (wide * factor * gain_ref[...].astype(F32)).astype(BF16)
    before = lax.broadcasted_iota(jnp.int32, (tokens, tokens), 0)
    after = lax.broadcasted_iota(jnp.int32, (tokens, tokens), 1)
    upper = jnp.where(before <= after, 1.0, 0.0).astype(BF16)

    def selection(j):
        named = (routes_ref[0:1, :] == j) | (routes_ref[1:2, :] == j)
        member = jnp.where(named, 1.0, 0.0)
        wide_member = jnp.broadcast_to(member, (8, tokens)).astype(BF16)
        ranks = jnp.dot(wide_member, upper, preferred_element_type=F32)[0:1, :]
        ranks = jnp.where(named, ranks, 0.0)
        places = lax.broadcasted_iota(jnp.int32, (cap, tokens), 0).astype(F32) + 1.0
        return jnp.where(places == ranks, 1.0, 0.0)

    def z_copy(k, slot):
        return remote(
            outgo.at[k, sent], rows.at[slot, mine, sent], z_send.at[k], z_recv.at[k],
            {"ep": peer(k)},
        )

    def picked_rows(j):
        return jnp.dot(selection(j).astype(BF16), normed, preferred_element_type=F32).astype(BF16)

    def forward_x(s):
        block = rows.at[s, mine, sent]
        return remote(block, block, fx_send.at[s], fx_recv.at[s], {"tp": over})

    def forward_c(s):
        block = rows.at[s, mine, sent]
        return remote(block, block, fc_send.at[s], fc_recv.at[s], {"tp": mate})

    def forward_d(s):
        block = rows.at[s, mine_over, sent]
        return remote(block, block, fd_send.at[s], fd_recv.at[s], {"tp": mate})

    @pl.loop(1, n_ep)
    def _(k):
        outgo[k, sent] = picked_rows(peer(k))
        z_copy(k, e).start()

    rows[e, mine, sent] = picked_rows(e)

    def head_mask(width, h, rows_count):
        lane = lax.broadcasted_iota(jnp.int32, (rows_count, width * heads), 1)
        return (lane >= h * width) & (lane < (h + 1) * width)

    heads = kw_ref.shape[1] // PLAIN_DIM
    queries = q_ref.shape[0]
    quarter = lat_ref.shape[0]
    latent_width = kw_ref.shape[0]
    rotary_width = heads * ROTARY_DIM
    scale = (PLAIN_DIM + ROTARY_DIM) ** (-0.5)

    def head_c():
        return remote(head_part.at[1 - core], head_near, h_send, h_recv, {"tp": mate})

    def head_x():
        return remote(head_pair, head_across, i_send, i_recv, {"tp": over})

    def attend():
        @pl.loop(1, n_ep)
        def _(k):
            s = peer(k)
            lat_z(k, s).wait_recv()
            lat_x(s, lats.at[s, t]).start()
            lat_c(s, lats.at[s, t]).start()

        @pl.loop(0, n_ep)
        def _(k):
            s = peer(k)
            lat_x(s, lats.at[s, t]).wait_recv()
            lat_d(s).start()

        @pl.loop(0, n_ep)
        def _(k):
            s = peer(k)
            lat_c(s, lats.at[s, t]).wait_recv()
            lat_d(s).wait_recv()

        total[...] = jnp.zeros_like(total)
        highest[...] = jnp.full_like(highest, LOWEST)

        @pl.loop(0, n_ep)
        def _(s):
            @pl.when(s <= e)
            def _():
                piece = lats[s].reshape(n_tp * quarter, lat_ref.shape[1])
                latent = piece[:, :latent_width]
                turned = piece[:, latent_width : latent_width + rotary_width]
                keys = jnp.dot(latent, kw_ref[...], preferred_element_type=F32).astype(BF16)
                values = jnp.dot(latent, vw_ref[...], preferred_element_type=F32).astype(BF16)
                shape = (queries, n_tp * quarter)
                at_query = e * queries + lax.broadcasted_iota(jnp.int32, shape, 0)
                at_key = s * queries + lax.broadcasted_iota(jnp.int32, shape, 1)
                allowed = at_key <= at_query
                for h in range(heads):
                    plain = jnp.where(head_mask(PLAIN_DIM, h, queries), q_ref[...].astype(F32), 0.0).astype(BF16)
                    rot = jnp.where(head_mask(ROTARY_DIM, h, queries), qr_ref[...].astype(F32), 0.0).astype(BF16)
                    contract = (((1,), (1,)), ((), ()))
                    scores = lax.dot_general(plain, keys, contract, preferred_element_type=F32)
                    scores += lax.dot_general(rot, turned, contract, preferred_element_type=F32)
                    masked = jnp.where(allowed, scores * scale, LOWEST)
                    old = highest[h]
                    new = jnp.maximum(old, jnp.max(masked, axis=-1, keepdims=True))
                    weights = jnp.where(allowed, jnp.exp(masked - new[:, 0:1]), 0.0).astype(BF16)
                    total[h] = total[h] * jnp.exp(old - new) + jnp.dot(
                        weights, values, preferred_element_type=F32
                    )
                    highest[h] = new

        context = jnp.zeros((queries, heads * VALUE_DIM), F32)
        for h in range(heads):
            inside = head_mask(VALUE_DIM, h, queries)
            own = jnp.where(inside, total[h], 0.0)
            square = jnp.sum(own * own, axis=-1, keepdims=True) * (1.0 / VALUE_DIM)
            context = context + own * lax.rsqrt(square + EPSILON)
        head_output = (context * hgain_ref[...].astype(F32)).astype(BF16)
        share = jnp.dot(head_output, ow_ref[...], preferred_element_type=F32).astype(BF16)
        for other in range(n_tp):
            head_part[other % 2, other // 2] = share[other * quarter : (other + 1) * quarter]
        head_c().start()

    def multiply(s):
        piece = rows.at[s]
        stacked = n_tp * pitch

        @pl.loop(0, tiles)
        def _(n):
            both = jnp.dot(
                piece[...].reshape(stacked, features), wgu[n], preferred_element_type=F32
            )
            gate = both[:, :LANES]
            hidden[:, pl.ds(pl.multiple_of(n * LANES, LANES), LANES)] = (
                gate / (1.0 + jnp.exp(-gate)) * both[:, LANES:]
            ).astype(BF16)

        step = 2 * LANES

        @pl.loop(0, features // step)
        def _(n):
            columns = pl.ds(pl.multiple_of(n * step, step), step)
            result = jnp.dot(hidden[...], wd[:, columns], preferred_element_type=F32)
            part[s, :, :, :, columns] = result.astype(BF16).reshape(2, outer, pitch, step)

    def near_copy(s):
        return remote(
            part.at[s, 1 - core, :, sent], near.at[s, :, sent], n_send.at[s], n_recv.at[s],
            {"tp": mate},
        )

    def across_copy(s):
        return remote(
            pair.at[s, sent], across.at[s, sent], a_send.at[s], a_recv.at[s], {"tp": over}
        )

    def back_copy(k, slot):
        s = peer(k)
        return remote(
            done.at[s, sent], back.at[slot, sent], b_send.at[k], b_recv.at[k], {"ep": s}
        )

    @pl.loop(0, n_ep + 5)
    def _(it):
        @pl.when((it >= 2) & (it < n_ep + 2))
        def _():
            s = peer(it - 2)
            forward_c(s).wait_recv()
            forward_d(s).wait_recv()

            @pl.when(it == 2)
            def _():
                for n in range(tiles):
                    for copy in tile_copies(n):
                        copy.wait()
                down_copy.wait()

            multiply(s)
            near_copy(s).start()

        @pl.when((it >= 3) & (it < n_ep + 3))
        def _():
            s = peer(it - 3)
            near_copy(s).wait_recv()
            pair[s, sent] = (
                part[s, core, 1 - side, sent].astype(F32) + near[s, 1 - side, sent].astype(F32)
            ).astype(BF16)
            across_copy(s).start()

        @pl.when(it == 2)
        def _():
            head_c().wait_recv()
            head_pair[...] = (
                head_part[core, 1 - side].astype(F32) + head_near[1 - side].astype(F32)
            ).astype(BF16)
            head_x().start()

        @pl.when((it >= 1) & (it < n_ep + 1))
        def _():
            s = peer(it - 1)
            forward_x(s).wait_recv()
            forward_d(s).start()

        @pl.when((it >= 4) & (it < n_ep + 4))
        def _():
            k = it - 4
            s = peer(k)
            across_copy(s).wait_recv()
            final = (
                part[s, core, side, sent].astype(F32)
                + near[s, side, sent].astype(F32)
                + across[s, sent].astype(F32)
            ).astype(BF16)

            @pl.when(k == 0)
            def _():
                back[e, sent] = final

            @pl.when(k > 0)
            def _():
                done[s, sent] = final
                back_copy(k, e).start()

        @pl.when(it < n_ep)
        def _():
            s = peer(it)

            @pl.when(it > 0)
            def _():
                z_copy(it, s).wait_recv()

            forward_x(s).start()
            forward_c(s).start()

        @pl.when(it == 0)
        def _():
            attend()

    head_x().wait_recv()
    att_ref[...] = (
        head_part[core, side].astype(F32)
        + head_near[side].astype(F32)
        + head_across[...].astype(F32)
    ).astype(BF16)

    def gathered(k, acc):
        s = peer(k)

        @pl.when(k > 0)
        def _():
            back_copy(k, s).wait_recv()

        scaled = jnp.where(routes_ref[0:1, :] == s, weight_ref[0:1, :], 0.0)
        scaled = scaled + jnp.where(routes_ref[1:2, :] == s, weight_ref[1:2, :], 0.0)
        spread = selection(s) * scaled
        high = spread.astype(BF16)
        low = (spread - high.astype(F32)).astype(BF16)
        contract = (((0,), (0,)), ((), ()))
        block = back[s, sent]
        acc[...] += lax.dot_general(high, block, contract, preferred_element_type=F32)
        acc[...] += lax.dot_general(low, block, contract, preferred_element_type=F32)

    def combine(acc):
        acc[...] = jnp.zeros_like(acc)

        @pl.loop(0, n_ep)
        def _(k):
            gathered(k, acc)

        out_ref[...] = acc[...].astype(BF16)

    pl.run_scoped(combine, pltpu.VMEM((tokens, features), F32))

    @pl.loop(0, n_ep)
    def _(k):
        s = peer(k)

        @pl.when(k > 0)
        def _():
            z_copy(k, e).wait_send()
            lat_z(k, e).wait_send()
            back_copy(k, e).wait_send()

        forward_x(s).wait_send()
        forward_c(s).wait_send()
        forward_d(s).wait_send()
        near_copy(s).wait_send()
        across_copy(s).wait_send()
        lat_x(s, lats.at[s, t]).wait_send()
        lat_c(s, lats.at[s, t]).wait_send()
        lat_d(s).wait_send()

    head_c().wait_send()
    head_x().wait_send()


def body(
    query_plain, query_rotary, latent_input, rotary_key, key_weight, value_weight, latent_gain,
    head_gain, out_weight, expert_input, expert_gain, routes, route_weight, gate_weight,
    up_weight, down_weight,
):
    n_ep, n_tp = lax.axis_size("ep"), lax.axis_size("tp")
    e, t = lax.axis_index("ep"), lax.axis_index("tp")
    tokens, features = expert_input.shape
    count = query_plain.shape[0]
    quarter = count // n_tp
    heads = key_weight.shape[1] // PLAIN_DIM
    capacity = min(tokens, max(2, (9 * tokens + 4 * n_ep - 1) // (4 * n_ep)))
    cap = -(-capacity // 8) * 8
    pitch = -(-cap // 16) * 16
    units = gate_weight.shape[2]
    tiles = units // LANES

    own = lax.dynamic_slice_in_dim(latent_input, t * quarter, quarter, 0)
    own_key = lax.dynamic_slice_in_dim(rotary_key, t * quarter, quarter, 0)
    own_positions = e * count + t * quarter + jnp.arange(quarter, dtype=jnp.int32)
    latent = normalize(own, latent_gain).astype(BF16)
    turned = rotate(own_key.reshape(quarter, 1, ROTARY_DIM), own_positions).reshape(
        quarter, ROTARY_DIM
    )
    width = latent.shape[1] + heads * ROTARY_DIM
    padded = -(-width // LANES) * LANES
    packed = jnp.concatenate(
        [latent] + [turned] * heads + [jnp.zeros((quarter, padded - width), BF16)], axis=1
    )
    positions = e * count + jnp.arange(count, dtype=jnp.int32)
    query_rotated = rotate(query_rotary.reshape(count, heads, ROTARY_DIM), positions).reshape(
        count, heads * ROTARY_DIM
    )

    dma = pltpu.SemaphoreType.DMA
    vmem = pl.BlockSpec(memory_space=pltpu.VMEM)
    far = pl.BlockSpec(memory_space=pl.ANY)
    outer = n_tp // 2
    block = (pitch, features)
    attended, expert_out = pl.pallas_call(
        functools.partial(kernel, (n_ep, n_tp, cap)),
        out_shape=(
            jax.ShapeDtypeStruct((quarter, features), BF16),
            jax.ShapeDtypeStruct((tokens, features), BF16),
        ),
        in_specs=[vmem] * 11 + [far] * 3,
        out_specs=(vmem, vmem),
        scratch_shapes=[
            pltpu.VMEM((tiles, features, 2 * LANES), BF16),
            pltpu.VMEM((units, features), BF16),
            pltpu.VMEM((n_ep,) + block, BF16),
            pltpu.VMEM((n_ep, n_tp) + block, BF16),
            pltpu.VMEM((n_ep, 2, outer) + block, BF16),
            pltpu.VMEM((n_tp * pitch, units), BF16),
            pltpu.VMEM((n_ep, outer) + block, BF16),
            pltpu.VMEM((n_ep,) + block, BF16),
            pltpu.VMEM((n_ep,) + block, BF16),
            pltpu.VMEM((n_ep,) + block, BF16),
            pltpu.VMEM((n_ep,) + block, BF16),
            pltpu.VMEM((n_ep, n_tp, quarter, padded), BF16),
            pltpu.VMEM((heads, count, heads * VALUE_DIM), F32),
            pltpu.VMEM((heads, count, LANES), F32),
            pltpu.VMEM((2, outer, quarter, features), BF16),
            pltpu.VMEM((outer, quarter, features), BF16),
            pltpu.VMEM((quarter, features), BF16),
            pltpu.VMEM((quarter, features), BF16),
            dma((2 * tiles + 1,)),
        ]
        + [dma((n_ep,))] * 22
        + [dma] * 4,
        compiler_params=pltpu.CompilerParams(
            collective_id=0, has_side_effects=True, vmem_limit_bytes=60 * 1024 * 1024
        ),
    )(
        expert_input, expert_gain.reshape(1, -1), routes.T, route_weight.T, packed,
        query_plain, query_rotated, key_weight, value_weight, head_gain.reshape(1, -1),
        out_weight, gate_weight, up_weight, down_weight,
    )
    return (attended, expert_out)


def solution(mesh):
    return jax.shard_map(
        body,
        mesh=mesh,
        in_specs=(
            P(("grp", "ep"), "tp"),
            P(("grp", "ep"), "tp"),
            P(("grp", "ep"), None),
            P(("grp", "ep"), None),
            P(None, "tp"),
            P(None, "tp"),
            P(),
            P("tp"),
            P("tp", None),
            P(("grp", "ep", "tp"), None),
            P(),
            P(("grp", "ep", "tp"), None),
            P(("grp", "ep", "tp"), None),
            P("ep", None, "tp"),
            P("ep", None, "tp"),
            P("ep", "tp", None),
        ),
        out_specs=(P(("grp", "ep", "tp"), None), P(("grp", "ep", "tp"), None)),
        check_vma=False,
    )
```

```python
import functools
import math
import jax
import jax.numpy as jnp
from jax import lax
from jax.experimental import pallas as pl
from jax.experimental.pallas import tpu as pltpu
from jax.sharding import PartitionSpec as P

PLAIN_DIM = 64
ROTARY_DIM = 32
VALUE_DIM = 64
EPSILON = 1e-06
THETA = 10000.0
LOWEST = -1e30
LANES = 128
MESH = pl.DeviceIdType.MESH
F32 = jnp.float32
BF16 = jnp.bfloat16


def kernel(
    dims,
    x_ref, gain_ref, routes_ref, weight_ref, latent_ref, rk_ref, lgain_ref, q_ref, qraw_ref, kw_ref, vw_ref,
    hgain_ref, ow_ref, gate_hbm, up_hbm, down_hbm,
    att_ref, out_ref,
    wgu, wd, outgo, rows, part, hidden, near, pair, across, done, back,
    lats, lat_ref, qr_ref, total, highest, head_part, head_near, head_pair, head_across,
    w_sem, z_send, z_recv, fx_send, fx_recv, fc_send, fc_recv, fd_send, fd_recv,
    n_send, n_recv, a_send, a_recv, b_send, b_recv,
    lz_send, lz_recv, lx_send, lx_recv, lc_send, lc_recv, ld_send, ld_recv,
    h_send, h_recv, i_send, i_recv,
):
    n_ep, n_tp, cap = dims
    tokens = x_ref.shape[0]
    features = x_ref.shape[1]
    tiles = wgu.shape[0]
    pitch = rows.shape[2]
    outer = n_tp // 2
    e = lax.axis_index("ep")
    t = lax.axis_index("tp")
    core = lax.rem(t, 2)
    side = t // 2
    mate = t + 1 - 2 * core
    over = lax.rem(t + 2, n_tp)
    mine = core * outer + side
    mine_over = core * outer + (1 - side)
    sent = pl.ds(0, cap)

    def peer(k):
        return lax.bitwise_xor(e, k)

    def remote(src, dst, send, recv, where):
        return pltpu.make_async_remote_copy(
            src_ref=src, dst_ref=dst, send_sem=send, recv_sem=recv,
            device_id=where, device_id_type=MESH,
        )

    def tile_copies(n):
        columns = pl.ds(n * LANES, LANES)
        return (
            pltpu.make_async_copy(
                gate_hbm.at[0, :, columns], wgu.at[n, :, pl.ds(0, LANES)], w_sem.at[2 * n]
            ),
            pltpu.make_async_copy(
                up_hbm.at[0, :, columns], wgu.at[n, :, pl.ds(LANES, LANES)], w_sem.at[2 * n + 1]
            ),
        )

    down_copy = pltpu.make_async_copy(down_hbm.at[0], wd, w_sem.at[2 * tiles])
    for n in range(tiles):
        for copy in tile_copies(n):
            copy.start()
    down_copy.start()

    barrier = pltpu.get_barrier_semaphore()

    @pl.loop(1, n_ep)
    def _(k):
        pl.semaphore_signal(barrier, inc=1, device_id={"ep": peer(k)}, device_id_type=MESH)

    for where in (mate, over):
        pl.semaphore_signal(barrier, inc=1, device_id={"tp": where}, device_id_type=MESH)
    pl.semaphore_wait(barrier, n_ep + 1)

    def lat_z(k, slot):
        return remote(lat_ref, lats.at[slot, t], lz_send.at[k], lz_recv.at[k], {"ep": peer(k)})

    def lat_x(s, src):
        return remote(src, lats.at[s, t], lx_send.at[s], lx_recv.at[s], {"tp": over})

    def lat_c(s, src):
        return remote(src, lats.at[s, t], lc_send.at[s], lc_recv.at[s], {"tp": mate})

    def lat_d(s):
        return remote(
            lats.at[s, over], lats.at[s, over], ld_send.at[s], ld_recv.at[s], {"tp": mate}
        )

    half = ROTARY_DIM // 2

    def turn(values, repeats, first_position):
        count, width = values.shape
        wide_width = width * repeats
        lane = lax.broadcasted_iota(jnp.int32, (1, wide_width), 1)
        step = jnp.exp((lane & (half - 1)).astype(F32) * (-math.log(THETA) / half))
        place = first_position + lax.broadcasted_iota(jnp.int32, (count, 1), 0)
        angle = place.astype(F32) * step
        source = lax.broadcasted_iota(jnp.int32, (width, wide_width), 0)
        target = lax.broadcasted_iota(jnp.int32, (width, wide_width), 1)
        target = target & (width - 1)
        low = (target & half) == 0
        plain = jnp.where(source == target, 1.0, 0.0).astype(BF16)
        crossed = jnp.where(
            low & (source == target + half), -1.0,
            jnp.where((~low) & (source == target - half), 1.0, 0.0),
        ).astype(BF16)
        straight = jnp.dot(values, plain, preferred_element_type=F32)
        other = jnp.dot(values, crossed, preferred_element_type=F32)
        return (straight * jnp.cos(angle) + other * jnp.sin(angle)).astype(BF16)

    heads = kw_ref.shape[1] // PLAIN_DIM
    queries = q_ref.shape[0]
    quarter = lat_ref.shape[0]
    latent_width = kw_ref.shape[0]
    rotary_width = heads * ROTARY_DIM
    scale = (PLAIN_DIM + ROTARY_DIM) ** (-0.5)
    own_range = pl.ds(pl.multiple_of(t * quarter, quarter), quarter)
    own_latent = latent_ref[own_range, :].astype(F32)
    own_factor = lax.rsqrt(jnp.mean(own_latent * own_latent, axis=-1, keepdims=True) + EPSILON)
    lat_ref[:, :latent_width] = (
        own_latent * own_factor * lgain_ref[...].astype(F32)[None, :]
    ).astype(BF16)
    lat_ref[:, latent_width : latent_width + rotary_width] = turn(
        rk_ref[own_range, :], heads, e * queries + t * quarter
    )
    lats[e, t] = lat_ref[...]

    @pl.loop(1, n_ep)
    def _(k):
        lat_z(k, e).start()

    lat_x(e, lat_ref).start()
    lat_c(e, lat_ref).start()

    wide = x_ref[...].astype(F32)
    factor = lax.rsqrt(jnp.mean(wide * wide, axis=-1, keepdims=True) + EPSILON)
    normed = (wide * factor * gain_ref[...].astype(F32)[None, :]).astype(BF16)
    before = lax.broadcasted_iota(jnp.int32, (tokens, tokens), 0)
    after = lax.broadcasted_iota(jnp.int32, (tokens, tokens), 1)
    upper = jnp.where(before <= after, 1.0, 0.0).astype(BF16)

    def selection(j):
        named = (routes_ref[0:1, :] == j) | (routes_ref[1:2, :] == j)
        member = jnp.where(named, 1.0, 0.0)
        wide_member = jnp.broadcast_to(member, (8, tokens)).astype(BF16)
        ranks = jnp.dot(wide_member, upper, preferred_element_type=F32)[0:1, :]
        ranks = jnp.where(named, ranks, 0.0)
        places = lax.broadcasted_iota(jnp.int32, (cap, tokens), 0).astype(F32) + 1.0
        return jnp.where(places == ranks, 1.0, 0.0)

    def z_copy(k, slot):
        return remote(
            outgo.at[k, sent], rows.at[slot, mine, sent], z_send.at[k], z_recv.at[k],
            {"ep": peer(k)},
        )

    def picked_rows(j):
        return jnp.dot(selection(j).astype(BF16), normed, preferred_element_type=F32).astype(BF16)

    def forward_x(s):
        block = rows.at[s, mine, sent]
        return remote(block, block, fx_send.at[s], fx_recv.at[s], {"tp": over})

    def forward_c(s):
        block = rows.at[s, mine, sent]
        return remote(block, block, fc_send.at[s], fc_recv.at[s], {"tp": mate})

    def forward_d(s):
        block = rows.at[s, mine_over, sent]
        return remote(block, block, fd_send.at[s], fd_recv.at[s], {"tp": mate})

    order = []
    span = n_ep
    while span > 1:
        order += list(range(span // 2, span))
        span //= 2
    own_rows = picked_rows(e)
    rows[e, mine, sent] = own_rows
    for k in range(1, n_ep):
        outgo[k, sent] = picked_rows(peer(k))
        z_copy(k, e).start()

    forward_x(e).start()
    forward_c(e).start()

    qr_ref[...] = turn(qraw_ref[...], 1, e * queries)

    def head_mask(width, h, rows_count):
        lane = lax.broadcasted_iota(jnp.int32, (rows_count, width * heads), 1)
        return (lane >= h * width) & (lane < (h + 1) * width)

    def head_c():
        return remote(head_part.at[1 - core], head_near, h_send, h_recv, {"tp": mate})

    def head_x():
        return remote(head_pair, head_across, i_send, i_recv, {"tp": over})

    def attend():
        @pl.loop(1, n_ep)
        def _(k):
            s = peer(k)
            lat_z(k, s).wait_recv()
            lat_x(s, lats.at[s, t]).start()
            lat_c(s, lats.at[s, t]).start()

        @pl.loop(0, n_ep)
        def _(k):
            s = peer(k)
            lat_x(s, lats.at[s, t]).wait_recv()
            lat_d(s).start()

        @pl.loop(0, n_ep)
        def _(k):
            s = peer(k)
            lat_c(s, lats.at[s, t]).wait_recv()
            lat_d(s).wait_recv()

        total[...] = jnp.zeros_like(total)
        highest[...] = jnp.full_like(highest, LOWEST)

        @pl.loop(0, n_ep)
        def _(s):
            @pl.when(s <= e)
            def _():
                piece = lats[s].reshape(n_tp * quarter, lat_ref.shape[1])
                latent = piece[:, :latent_width]
                turned = piece[:, latent_width : latent_width + rotary_width]
                keys = jnp.dot(latent, kw_ref[...], preferred_element_type=F32).astype(BF16)
                values = jnp.dot(latent, vw_ref[...], preferred_element_type=F32).astype(BF16)
                shape = (queries, n_tp * quarter)
                at_query = e * queries + lax.broadcasted_iota(jnp.int32, shape, 0)
                at_key = s * queries + lax.broadcasted_iota(jnp.int32, shape, 1)
                allowed = at_key <= at_query
                for h in range(heads):
                    plain = jnp.where(head_mask(PLAIN_DIM, h, queries), q_ref[...].astype(F32), 0.0).astype(BF16)
                    rot = jnp.where(head_mask(ROTARY_DIM, h, queries), qr_ref[...].astype(F32), 0.0).astype(BF16)
                    contract = (((1,), (1,)), ((), ()))
                    scores = lax.dot_general(plain, keys, contract, preferred_element_type=F32)
                    scores += lax.dot_general(rot, turned, contract, preferred_element_type=F32)
                    masked = jnp.where(allowed, scores * scale, LOWEST)
                    old = highest[h]
                    new = jnp.maximum(old, jnp.max(masked, axis=-1, keepdims=True))
                    weights = jnp.where(allowed, jnp.exp(masked - new[:, 0:1]), 0.0).astype(BF16)
                    total[h] = total[h] * jnp.exp(old - new) + jnp.dot(
                        weights, values, preferred_element_type=F32
                    )
                    highest[h] = new

        context = jnp.zeros((queries, heads * VALUE_DIM), F32)
        for h in range(heads):
            inside = head_mask(VALUE_DIM, h, queries)
            own = jnp.where(inside, total[h], 0.0)
            square = jnp.sum(own * own, axis=-1, keepdims=True) * (1.0 / VALUE_DIM)
            context = context + own * lax.rsqrt(square + EPSILON)
        head_output = (context * hgain_ref[...].astype(F32)[None, :]).astype(BF16)
        share = jnp.dot(head_output, ow_ref[...], preferred_element_type=F32).astype(BF16)
        for other in range(n_tp):
            head_part[other % 2, other // 2] = share[other * quarter : (other + 1) * quarter]
        head_c().start()

    def multiply(s):
        piece = rows.at[s]
        stacked = n_tp * pitch

        @pl.loop(0, tiles)
        def _(n):
            both = jnp.dot(
                piece[...].reshape(stacked, features), wgu[n], preferred_element_type=F32
            )
            gate = both[:, :LANES]
            hidden[:, pl.ds(pl.multiple_of(n * LANES, LANES), LANES)] = (
                gate / (1.0 + jnp.exp(-gate)) * both[:, LANES:]
            ).astype(BF16)

        step = 2 * LANES

        @pl.loop(0, features // step)
        def _(n):
            columns = pl.ds(pl.multiple_of(n * step, step), step)
            result = jnp.dot(hidden[...], wd[:, columns], preferred_element_type=F32)
            part[s, :, :, :, columns] = result.astype(BF16).reshape(2, outer, pitch, step)

    def near_copy(s):
        return remote(
            part.at[s, 1 - core, :, sent], near.at[s, :, sent], n_send.at[s], n_recv.at[s],
            {"tp": mate},
        )

    def across_copy(s):
        return remote(
            pair.at[s, sent], across.at[s, sent], a_send.at[s], a_recv.at[s], {"tp": over}
        )

    def back_copy(k, slot):
        s = peer(k)
        return remote(
            done.at[s, sent], back.at[slot, sent], b_send.at[k], b_recv.at[k], {"ep": s}
        )

    def arrive(k):
        s = peer(k)
        z_copy(k, s).wait_recv()
        forward_x(s).start()
        forward_c(s).start()

    def relay(k):
        s = peer(k)
        forward_x(s).wait_recv()
        forward_d(s).start()

    def expert(k):
        s = peer(k)
        forward_c(s).wait_recv()
        forward_d(s).wait_recv()
        multiply(s)
        near_copy(s).start()

    def add_near(k):
        s = peer(k)
        near_copy(s).wait_recv()
        pair[s, sent] = (
            part[s, core, 1 - side, sent].astype(F32) + near[s, 1 - side, sent].astype(F32)
        ).astype(BF16)
        across_copy(s).start()

    def finish(k):
        s = peer(k)
        across_copy(s).wait_recv()
        final = (
            part[s, core, side, sent].astype(F32)
            + near[s, side, sent].astype(F32)
            + across[s, sent].astype(F32)
        ).astype(BF16)
        if k == 0:
            back[e, sent] = final
        else:
            done[s, sent] = final
            back_copy(k, e).start()

    attend()
    relay(0)
    for n in range(tiles):
        for copy in tile_copies(n):
            copy.wait()
    down_copy.wait()
    head_c().wait_recv()
    head_pair[...] = (
        head_part[core, 1 - side].astype(F32) + head_near[1 - side].astype(F32)
    ).astype(BF16)
    head_x().start()
    expert(0)
    arrive(order[0])
    add_near(0)
    relay(order[0])
    expert(order[0])
    for i in range(1, len(order)):
        last = i == len(order) - 1
        if not last or i == 0:
            arrive(order[i])
        add_near(order[i - 1])
        if i == len(order) - 2:
            arrive(order[i + 1])
        relay(order[i])
        expert(order[i])
        finish(order[i - 1])
    add_near(order[-1])
    finish(order[-1])
    finish(0)

    head_x().wait_recv()
    att_ref[...] = (
        head_part[core, side].astype(F32)
        + head_near[side].astype(F32)
        + head_across[...].astype(F32)
    ).astype(BF16)

    def gathered(k, acc):
        s = peer(k)
        if k > 0:
            back_copy(k, s).wait_recv()

        scaled = jnp.where(routes_ref[0:1, :] == s, weight_ref[0:1, :], 0.0)
        scaled = scaled + jnp.where(routes_ref[1:2, :] == s, weight_ref[1:2, :], 0.0)
        spread = selection(s) * scaled
        high = spread.astype(BF16)
        low = (spread - high.astype(F32)).astype(BF16)
        contract = (((0,), (0,)), ((), ()))
        block = back[s, sent]
        acc[...] += lax.dot_general(high, block, contract, preferred_element_type=F32)
        acc[...] += lax.dot_general(low, block, contract, preferred_element_type=F32)

    def combine(acc):
        acc[...] = jnp.zeros_like(acc)

        for k in [0] + order:
            gathered(k, acc)
        out_ref[...] = acc[...].astype(BF16)

    pl.run_scoped(combine, pltpu.VMEM((tokens, features), F32))

    @pl.loop(0, n_ep)
    def _(k):
        s = peer(k)

        @pl.when(k > 0)
        def _():
            z_copy(k, e).wait_send()
            lat_z(k, e).wait_send()
            back_copy(k, e).wait_send()

        forward_x(s).wait_send()
        forward_c(s).wait_send()
        forward_d(s).wait_send()
        near_copy(s).wait_send()
        across_copy(s).wait_send()
        lat_x(s, lats.at[s, t]).wait_send()
        lat_c(s, lats.at[s, t]).wait_send()
        lat_d(s).wait_send()

    head_c().wait_send()
    head_x().wait_send()


def body(
    query_plain, query_rotary, latent_input, rotary_key, key_weight, value_weight, latent_gain,
    head_gain, out_weight, expert_input, expert_gain, routes, route_weight, gate_weight,
    up_weight, down_weight,
):
    n_ep, n_tp = lax.axis_size("ep"), lax.axis_size("tp")
    e, t = lax.axis_index("ep"), lax.axis_index("tp")
    tokens, features = expert_input.shape
    count = query_plain.shape[0]
    quarter = count // n_tp
    heads = key_weight.shape[1] // PLAIN_DIM
    capacity = min(tokens, max(2, (9 * tokens + 4 * n_ep - 1) // (4 * n_ep)))
    cap = -(-capacity // 8) * 8
    pitch = -(-cap // 16) * 16
    units = gate_weight.shape[2]
    tiles = units // LANES

    width = latent_input.shape[1] + heads * ROTARY_DIM
    padded = -(-width // LANES) * LANES

    dma = pltpu.SemaphoreType.DMA
    vmem = pl.BlockSpec(memory_space=pltpu.VMEM)
    far = pl.BlockSpec(memory_space=pl.ANY)
    outer = n_tp // 2
    block = (pitch, features)
    attended, expert_out = pl.pallas_call(
        functools.partial(kernel, (n_ep, n_tp, cap)),
        out_shape=(
            jax.ShapeDtypeStruct((quarter, features), BF16),
            jax.ShapeDtypeStruct((tokens, features), BF16),
        ),
        in_specs=[vmem] * 13 + [far] * 3,
        out_specs=(vmem, vmem),
        scratch_shapes=[
            pltpu.VMEM((tiles, features, 2 * LANES), BF16),
            pltpu.VMEM((units, features), BF16),
            pltpu.VMEM((n_ep,) + block, BF16),
            pltpu.VMEM((n_ep, n_tp) + block, BF16),
            pltpu.VMEM((n_ep, 2, outer) + block, BF16),
            pltpu.VMEM((n_tp * pitch, units), BF16),
            pltpu.VMEM((n_ep, outer) + block, BF16),
            pltpu.VMEM((n_ep,) + block, BF16),
            pltpu.VMEM((n_ep,) + block, BF16),
            pltpu.VMEM((n_ep,) + block, BF16),
            pltpu.VMEM((n_ep,) + block, BF16),
            pltpu.VMEM((n_ep, n_tp, quarter, padded), BF16),
            pltpu.VMEM((quarter, padded), BF16),
            pltpu.VMEM((count, heads * ROTARY_DIM), BF16),
            pltpu.VMEM((heads, count, heads * VALUE_DIM), F32),
            pltpu.VMEM((heads, count, LANES), F32),
            pltpu.VMEM((2, outer, quarter, features), BF16),
            pltpu.VMEM((outer, quarter, features), BF16),
            pltpu.VMEM((quarter, features), BF16),
            pltpu.VMEM((quarter, features), BF16),
            dma((2 * tiles + 1,)),
        ]
        + [dma((n_ep,))] * 22
        + [dma] * 4,
        compiler_params=pltpu.CompilerParams(
            collective_id=0, has_side_effects=True, vmem_limit_bytes=60 * 1024 * 1024
        ),
    )(
        expert_input, expert_gain, routes.T, route_weight.T, latent_input, rotary_key,
        latent_gain, query_plain, query_rotary, key_weight, value_weight, head_gain,
        out_weight, gate_weight, up_weight, down_weight,
    )
    return (attended, expert_out)


def solution(mesh):
    return jax.shard_map(
        body,
        mesh=mesh,
        in_specs=(
            P(("grp", "ep"), "tp"),
            P(("grp", "ep"), "tp"),
            P(("grp", "ep"), None),
            P(("grp", "ep"), None),
            P(None, "tp"),
            P(None, "tp"),
            P(),
            P("tp"),
            P("tp", None),
            P(("grp", "ep", "tp"), None),
            P(),
            P(("grp", "ep", "tp"), None),
            P(("grp", "ep", "tp"), None),
            P("ep", None, "tp"),
            P("ep", None, "tp"),
            P("ep", "tp", None),
        ),
        out_specs=(P(("grp", "ep", "tp"), None), P(("grp", "ep", "tp"), None)),
        check_vma=False,
    )
```
